32 devices in a mesh: sp: 8 (over z, y), dp: 4 (over x, core).
Axes of the slice: x: 2, y: 2, z: 4, core: 2. Of those that a mesh axis runs over, the one named last changes fastest.
Arguments:
- hidden_states: bfloat16 [8, 1024, 2048], P('dp', 'sp'), may hold values from -288 to 288
- cumulative_gate: float32 [8, 1024, 32], P('dp', 'sp'), may hold values from -4096 to 0, as said below
- query_weight: bfloat16 [2048, 2048], P('dp'), may hold values from -0.125 to 0.125
- key_weight: bfloat16 [2048, 512], P('dp'), may hold values from -0.125 to 0.125
- value_weight: bfloat16 [2048, 512], P('dp'), may hold values from -0.125 to 0.125
- out_weight: bfloat16 [2048, 2048], P('dp'), may hold values from -0.75 to 0.75
Outputs:
- mixed: bfloat16 [8, 1024, 2048], P('dp', 'sp')
The draws below stay inside these ranges and needn't reach their ends.
Inputs may be any that keep to these rules, and one draw needn't show every extreme that they name: cumulative_gate never rises along a sequence and is at most 0.
All inputs are finite; a program needn't handle non-finite values.
Results may differ from the reference program's by a relative error of at most 0.009.
The reference program's roundings to bfloat16 on the way (of `query`, `key`, `value`, `weights` and `attended`) count: a program that leaves them out, or rounds other values in their place, can miss the bound.
Values may be sent and summed in bfloat16 or wider, within the bound.
A program may use at most 64 MiB of HBM per device.

```python
import math
import jax
import jax.numpy as jnp
from jax import lax

D = 2048
HEADS = 32
KV_HEADS = 8
HEAD = 64
POS_DEV = 128
QW = 2048
KVW = 512
SEQUENCE_LENGTH = 1024
SEQS = 8


def draw_hidden_states(key, part):
    random_keys = jax.random.split(jax.random.fold_in(key, 3), 1)
    values = jnp.clip(jax.random.normal(random_keys[0], (SEQS, SEQUENCE_LENGTH, D), jnp.float32), -6.0, 6.0)
    return values.astype(jnp.bfloat16)


def draw_cumulative_gate(key, part):
    random_keys = jax.random.split(jax.random.fold_in(key, 7), 7)
    order = jax.random.permutation(random_keys[0], HEADS)
    sluggish_heads = order < HEADS // 2
    slow_rate = 0.5
    tensor_extent = (SEQS, SEQUENCE_LENGTH, HEADS)
    jaggedness = jax.random.uniform(random_keys[1], tensor_extent, jnp.float32, 0.3, 1.7)
    blocks = SEQUENCE_LENGTH // POS_DEV
    multiplier = jnp.exp(jax.random.uniform(random_keys[2], (SEQS, blocks, 1), jnp.float32, 0.0, math.log(4.0))) * 0.5
    multiplier = jnp.repeat(multiplier, POS_DEV, axis=1)
    forget_speed = jnp.where(sluggish_heads, slow_rate / SEQUENCE_LENGTH, 1.0 / 40.0)
    spike_events = (jax.random.uniform(random_keys[3], tensor_extent, jnp.float32) < 2.0 / SEQUENCE_LENGTH) & sluggish_heads
    spike_depth = jax.random.uniform(random_keys[4], tensor_extent, jnp.float32, 0.22, 0.7)
    quick_events = (jax.random.uniform(random_keys[5], tensor_extent, jnp.float32) < 1.0 / 16.0) & jnp.logical_not(sluggish_heads)
    quick_depth = jax.random.uniform(random_keys[6], tensor_extent, jnp.float32, 1.0, 3.0)
    gate_logarithm = -(forget_speed * jaggedness * multiplier + jnp.where(spike_events, spike_depth, 0.0) + jnp.where(quick_events, quick_depth, 0.0))
    return jnp.cumsum(gate_logarithm, axis=1).astype(jnp.float32)


def block_levels(own_key, dims, cuts, least, high):
    gain, own = 1.0, jax.random.fold_in(own_key, 6)
    for position, blocks in cuts:
        heights = jnp.exp(jax.random.uniform(jax.random.fold_in(own, position), (blocks,), jnp.float32, least / len(cuts), high / len(cuts)))
        gain = gain * jnp.repeat(heights, dims[position] // blocks).reshape([-1 if axis == position else 1 for axis in range(len(dims))])
    return gain


def noise(rng, extent, scale, bound, cuts=(), kind=jnp.bfloat16):
    array = scale * jax.random.normal(rng, extent, jnp.float32)
    if cuts:
        array = array * block_levels(rng, extent, cuts, -0.22, 0.18)
    return jnp.clip(array, -bound, bound).astype(kind)


def setup_inputs(seed: int = 0) -> dict:
    keys = jax.random.split(jax.random.key(seed), 7)
    return {
        "hidden_states": draw_hidden_states(jax.random.fold_in(keys[6], 71), 0),
        "cumulative_gate": draw_cumulative_gate(jax.random.fold_in(keys[6], 71), 0),
        "query_weight": noise(keys[2], (D, QW), D ** -0.5, 0.125, ((0, 4),)),
        "key_weight": noise(keys[3], (D, KVW), D ** -0.5, 0.125, ((0, 4),)),
        "value_weight": noise(keys[4], (D, KVW), D ** -0.5, 0.125, ((0, 4),)),
        "out_weight": noise(keys[5], (QW, D), (QW // 32) ** -0.5, 0.75, ((0, 4),)),
    }


def attend_one(query_head, key_head, value_head, gate_head):
    length = query_head.shape[0]
    block_rows = math.gcd(length, 512)
    block_count = length // block_rows
    key_index = jnp.arange(length, dtype=jnp.int32)
    scaling = query_head.shape[1] ** -0.5

    def one_block(block_number):
        offset = (block_number * block_rows).astype(jnp.int32)
        query_block = lax.dynamic_slice_in_dim(query_head, offset, block_rows, 0)
        gate_block = lax.dynamic_slice_in_dim(gate_head, offset, block_rows, 0)
        scores = jnp.dot(query_block, key_head.T, preferred_element_type=jnp.float32) * scaling
        scores = scores + gate_block[:, None] - gate_head[None, :]
        row_index = offset + jnp.arange(block_rows, dtype=jnp.int32)
        allowed = key_index[None, :] <= row_index[:, None]
        scores = jnp.where(allowed, scores, -jnp.inf)
        maximum = jnp.max(scores, axis=1, keepdims=True)
        exponent = jnp.where(allowed, jnp.exp(scores - maximum), 0.0)
        weights = (exponent / jnp.sum(exponent, axis=1, keepdims=True)).astype(jnp.bfloat16)
        return jnp.dot(weights, value_head, preferred_element_type=jnp.float32).astype(jnp.bfloat16)

    result = lax.map(one_block, jnp.arange(block_count, dtype=jnp.int32))
    return result.reshape(length, query_head.shape[1])


def reference(hidden_states, cumulative_gate, query_weight, key_weight, value_weight, out_weight):
    flattened = hidden_states.reshape(SEQS * SEQUENCE_LENGTH, D)
    query = jnp.dot(flattened, query_weight, preferred_element_type=jnp.float32).astype(jnp.bfloat16)
    query = query.reshape(SEQS, SEQUENCE_LENGTH, HEADS, HEAD)
    key = jnp.dot(flattened, key_weight, preferred_element_type=jnp.float32).astype(jnp.bfloat16)
    key = key.reshape(SEQS, SEQUENCE_LENGTH, KV_HEADS, HEAD)
    value = jnp.dot(flattened, value_weight, preferred_element_type=jnp.float32).astype(jnp.bfloat16)
    value = value.reshape(SEQS, SEQUENCE_LENGTH, KV_HEADS, HEAD)
    group_size = HEADS // KV_HEADS

    def per_sequence(inputs):
        seq_query, seq_key, seq_value, seq_gate = inputs

        def per_head(head_number):
            shared = head_number // group_size
            return attend_one(seq_query[:, head_number], seq_key[:, shared], seq_value[:, shared], seq_gate[:, head_number])

        return lax.map(per_head, jnp.arange(HEADS, dtype=jnp.int32))

    attended = lax.map(per_sequence, (query, key, value, cumulative_gate))
    attended = jnp.transpose(attended, (0, 2, 1, 3)).reshape(SEQS * SEQUENCE_LENGTH, QW)
    mixed = jnp.dot(attended, out_weight, preferred_element_type=jnp.float32).astype(jnp.bfloat16)
    return mixed.reshape(SEQS, SEQUENCE_LENGTH, D)
```

```python
import functools
import math

import jax
import jax.numpy as jnp
from jax import lax
from jax.experimental import pallas as pl
from jax.experimental.pallas import tpu as pltpu
from jax.sharding import PartitionSpec as P

KV_HEADS = 8
HEAD = 64


def attend_rows(q, k_of, v_of, gate_column, gate_row_of, start, rows):
    scaled = q * jnp.asarray(HEAD**-0.5, q.dtype)
    contract = (((1,), (1,)), ((), ()))

    def scores(lo, hi):
        product = lax.dot_general(scaled, k_of(lo, hi), contract, preferred_element_type=jnp.float32)
        return product + (gate_column - gate_row_of(lo, hi))

    diagonal = scores(start, start + rows)
    row = lax.broadcasted_iota(jnp.int32, diagonal.shape, 0)
    column = lax.broadcasted_iota(jnp.int32, diagonal.shape, 1)
    diagonal = jnp.where(column <= row, diagonal, -jnp.inf)
    top = jnp.max(diagonal, axis=1, keepdims=True)
    if start:
        before = scores(0, start)
        top = jnp.maximum(top, jnp.max(before, axis=1, keepdims=True))
    raised = jnp.exp(diagonal - top)
    total = jnp.sum(raised, axis=1, keepdims=True)
    mixed = jnp.dot(raised.astype(jnp.bfloat16), v_of(start, start + rows), preferred_element_type=jnp.float32)
    if start:
        raised = jnp.exp(before - top)
        total = total + jnp.sum(raised, axis=1, keepdims=True)
        mixed = mixed + jnp.dot(raised.astype(jnp.bfloat16), v_of(0, start), preferred_element_type=jnp.float32)
    return (mixed / total).astype(jnp.bfloat16)


def attention_kernel(per_pair, q_ref, k_ref, v_ref, gate_ref, row_ref, out_ref):
    length = q_ref.shape[1]
    heads = q_ref.shape[2] // HEAD
    rows = math.gcd(length, 256)
    if length <= 1024:
        for block in range(length // rows):
            start = block * rows
            for head in range(heads):
                pair = head // per_pair
                out_ref[0, start : start + rows, head * HEAD : (head + 1) * HEAD] = attend_rows(
                    q_ref[0, start : start + rows, head * HEAD : (head + 1) * HEAD],
                    lambda lo, hi: k_ref[0, lo:hi, pair * HEAD : (pair + 1) * HEAD],
                    lambda lo, hi: v_ref[0, lo:hi, pair * HEAD : (pair + 1) * HEAD],
                    gate_ref[0, start : start + rows, head : head + 1],
                    lambda lo, hi: row_ref[0, head : head + 1, lo:hi],
                    start,
                    rows,
                )
        return
    contract = (((1,), (1,)), ((), ()))
    for head in range(heads):
        pair = head // per_pair

        def one_block(block, nothing):
            start = pl.multiple_of(block * rows, rows)
            q = q_ref[0, pl.ds(start, rows), head * HEAD : (head + 1) * HEAD]
            scaled = q * jnp.asarray(HEAD**-0.5, q.dtype)
            column = gate_ref[0, pl.ds(start, rows), head : head + 1]

            def step(other, carry):
                top, total, mixed = carry
                lo = pl.multiple_of(other * rows, rows)
                k = k_ref[0, pl.ds(lo, rows), pair * HEAD : (pair + 1) * HEAD]
                v = v_ref[0, pl.ds(lo, rows), pair * HEAD : (pair + 1) * HEAD]
                s = lax.dot_general(scaled, k, contract, preferred_element_type=jnp.float32)
                s = s + (column - row_ref[0, head : head + 1, pl.ds(lo, rows)])
                at = lax.broadcasted_iota(jnp.int32, s.shape, 0) + start
                to = lax.broadcasted_iota(jnp.int32, s.shape, 1) + lo
                s = jnp.where(to <= at, s, -jnp.inf)
                new = jnp.maximum(top, jnp.max(s, axis=1, keepdims=True))
                raised = jnp.exp(s - new)
                keep = jnp.exp(top - new)
                total = total * keep + jnp.sum(raised, axis=1, keepdims=True)
                part = jnp.dot(raised.astype(jnp.bfloat16), v, preferred_element_type=jnp.float32)
                return new, total, mixed * keep + part

            first = (
                jnp.full((rows, 1), -jnp.inf, jnp.float32),
                jnp.zeros((rows, 1), jnp.float32),
                jnp.zeros((rows, HEAD), jnp.float32),
            )
            _, total, mixed = lax.fori_loop(0, block + 1, step, first)
            out_ref[0, pl.ds(start, rows), head * HEAD : (head + 1) * HEAD] = (mixed / total).astype(jnp.bfloat16)
            return nothing

        lax.fori_loop(0, length // rows, one_block, 0)


def attention(query, key, value, gates):
    sequences, length, width = query.shape
    heads = width // HEAD
    pairs = key.shape[2] // HEAD
    whole = lambda n, c: pl.BlockSpec((1, n, c), lambda i: (i, 0, 0))
    return pl.pallas_call(
        functools.partial(attention_kernel, heads // pairs),
        grid=(sequences,),
        out_shape=jax.ShapeDtypeStruct(query.shape, jnp.bfloat16),
        in_specs=[
            whole(length, width),
            whole(length, pairs * HEAD),
            whole(length, pairs * HEAD),
            whole(length, heads),
            whole(heads, length),
        ],
        out_specs=whole(length, width),
        compiler_params=pltpu.CompilerParams(vmem_limit_bytes=40 * 1024 * 1024),
    )(query, key, value, gates, jnp.swapaxes(gates, 1, 2))


def on_device(hidden_states, cumulative_gate, query_weight, key_weight, value_weight, out_weight):
    sequences, positions, model_width = hidden_states.shape
    rows = sequences * positions
    token_rows = hidden_states.reshape(rows, model_width)
    width_query = query_weight.shape[1]
    devices = lax.axis_size("sp")
    copies = max(1, devices // KV_HEADS)

    joined = jnp.concatenate([query_weight, key_weight, value_weight], axis=1)
    joined = lax.all_gather(joined, "dp", axis=0, tiled=True)
    summed = jnp.dot(token_rows, joined, preferred_element_type=jnp.float32).astype(jnp.bfloat16)
    width_key = key_weight.shape[1]

    def spread(matrix):
        matrix = matrix.reshape(sequences, positions, KV_HEADS, HEAD)
        return jnp.repeat(matrix, copies, axis=2).reshape(sequences, positions, devices, -1)

    parts = (
        summed[:, :width_query].reshape(sequences, positions, devices, -1),
        spread(summed[:, width_query : width_query + width_key]),
        spread(summed[:, width_query + width_key :]),
    )
    sent = jnp.concatenate(parts, axis=3)
    got = lax.all_to_all(sent, "sp", split_axis=2, concat_axis=1, tiled=True)
    got = got.reshape(sequences, positions * devices, -1)
    gates = lax.all_to_all(cumulative_gate, "sp", split_axis=2, concat_axis=1, tiled=True)
    own = parts[0].shape[3]
    pair = parts[1].shape[3]
    attended = attention(got[..., :own], got[..., own : own + pair], got[..., own + pair :], gates)
    returned = lax.all_to_all(attended, "sp", split_axis=1, concat_axis=2, tiled=True)
    mixed = jnp.dot(
        returned.reshape(rows, width_query),
        lax.all_gather(out_weight, "dp", axis=0, tiled=True),
        preferred_element_type=jnp.float32,
    )
    return mixed.astype(jnp.bfloat16).reshape(sequences, positions, model_width)


def solution(mesh):
    placed = (
        P("dp", "sp", None),
        P("dp", "sp", None),
        P("dp", None),
        P("dp", None),
        P("dp", None),
        P("dp", None),
    )
    return jax.shard_map(
        on_device, mesh=mesh, in_specs=placed, out_specs=P("dp", "sp", None), check_vma=False
    )
```

```python
import functools
import math

import jax
import jax.numpy as jnp
from jax import lax
from jax.experimental import pallas as pl
from jax.experimental.pallas import tpu as pltpu
from jax.sharding import PartitionSpec as P

KV_HEADS = 8
HEAD = 64


def attend_rows(q, k_of, v_of, gate_column, gate_row_of, start, rows):
    scaled = q * jnp.asarray(HEAD**-0.5, q.dtype)
    contract = (((1,), (1,)), ((), ()))

    def scores(lo, hi):
        product = lax.dot_general(scaled, k_of(lo, hi), contract, preferred_element_type=jnp.float32)
        return product + (gate_column - gate_row_of(lo, hi))

    diagonal = scores(start, start + rows)
    row = lax.broadcasted_iota(jnp.int32, diagonal.shape, 0)
    column = lax.broadcasted_iota(jnp.int32, diagonal.shape, 1)
    diagonal = jnp.where(column <= row, diagonal, -jnp.inf)
    top = jnp.max(diagonal, axis=1, keepdims=True)
    if start:
        before = scores(0, start)
        top = jnp.maximum(top, jnp.max(before, axis=1, keepdims=True))
    raised = jnp.exp(diagonal - top)
    total = jnp.sum(raised, axis=1, keepdims=True)
    mixed = jnp.dot(raised.astype(jnp.bfloat16), v_of(start, start + rows), preferred_element_type=jnp.float32)
    if start:
        raised = jnp.exp(before - top)
        total = total + jnp.sum(raised, axis=1, keepdims=True)
        mixed = mixed + jnp.dot(raised.astype(jnp.bfloat16), v_of(0, start), preferred_element_type=jnp.float32)
    return (mixed / total).astype(jnp.bfloat16)


def attend_long(q_of, k_of, v_of, gate_column_of, gate_row_of, store, length, rows):
    contract = (((1,), (1,)), ((), ()))

    def one_block(block, nothing):
        start = pl.multiple_of(block * rows, rows)
        q = q_of(start, rows)
        scaled = q * jnp.asarray(HEAD**-0.5, q.dtype)
        column = gate_column_of(start, rows)

        def step(other, carry):
            top, total, mixed = carry
            lo = pl.multiple_of(other * rows, rows)
            s = lax.dot_general(scaled, k_of(lo, rows), contract, preferred_element_type=jnp.float32)
            s = s + (column - gate_row_of(lo, rows))
            at = lax.broadcasted_iota(jnp.int32, s.shape, 0) + start
            to = lax.broadcasted_iota(jnp.int32, s.shape, 1) + lo
            s = jnp.where(to <= at, s, -jnp.inf)
            new = jnp.maximum(top, jnp.max(s, axis=1, keepdims=True))
            raised = jnp.exp(s - new)
            keep = jnp.exp(top - new)
            total = total * keep + jnp.sum(raised, axis=1, keepdims=True)
            part = jnp.dot(raised.astype(jnp.bfloat16), v_of(lo, rows), preferred_element_type=jnp.float32)
            return new, total, mixed * keep + part

        first = (
            jnp.full((rows, 1), -jnp.inf, jnp.float32),
            jnp.zeros((rows, 1), jnp.float32),
            jnp.zeros((rows, HEAD), jnp.float32),
        )
        _, total, mixed = lax.fori_loop(0, block + 1, step, first)
        store(block, (mixed / total).astype(jnp.bfloat16))
        return nothing

    lax.fori_loop(0, length // rows, one_block, 0)


class Gather:
    def __init__(self, buf, n, m, me, sems):
        self.buf, self.n, self.m = buf, n, m
        self.s, self.d = me
        self.have, self.partner_have, self.own_recv, self.send_a, self.send_b, self.send_c, self.own_send = sems
        self.partner = self.d + 1 - 2 * lax.rem(self.d, 2)
        self.y, self.z = lax.rem(self.s, 2), self.s // 2
        self.big = n // 2
        self.r1, self.r2 = split_rows(buf.shape[1], n)
        self.started = []
        self.mirrors = range(1, m // 2)

    def rows_pair(self, y):
        return pl.ds(pl.multiple_of(y * self.r1, 16), self.r1)

    def rows_many(self, z):
        return pl.ds(pl.multiple_of(2 * self.r1 + z * self.r2, 16), self.r2)

    def go(self, part, send, recv, device):
        copy = pltpu.make_async_remote_copy(
            src_ref=part, dst_ref=part, send_sem=send, recv_sem=recv, device_id=device,
            device_id_type=pl.DeviceIdType.MESH,
        )
        copy.start()
        self.started.append(copy)

    def take(self, part, recv):
        pltpu.make_async_remote_copy(
            src_ref=part, dst_ref=part, send_sem=self.own_send, recv_sem=recv, device_id=(self.s, self.partner),
            device_id_type=pl.DeviceIdType.MESH,
        ).wait_recv()

    def cross(self):
        for t in self.mirrors:
            to = (self.s, lax.rem(self.d + 2 * t, self.m))
            self.go(self.buf.at[self.d, self.rows_pair(self.y)], self.send_a.at[t, 0], self.have.at[t, self.y], to)
            if self.r2:
                self.go(
                    self.buf.at[self.d, self.rows_many(self.z)], self.send_a.at[t, 1], self.have.at[t, 2 + self.z], to
                )

    def to_partner(self):
        self.go(self.buf.at[self.d], self.own_send, self.own_recv, (self.s, self.partner))

    def take_partner(self):
        self.take(self.buf.at[self.partner], self.own_recv)

    def source(self, t):
        return lax.rem(self.d - 2 * t + self.m, self.m)

    def share(self):
        for t in self.mirrors:
            e = self.source(t)
            part = self.buf.at[e, self.rows_pair(self.y)]
            self.take(part, self.have.at[t, self.y])
            self.go(part, self.send_b.at[t, 0], self.have.at[t, self.y], (self.s + 1 - 2 * self.y, self.d))
            if self.r2:
                part = self.buf.at[e, self.rows_many(self.z)]
                self.take(part, self.have.at[t, 2 + self.z])
                for k in range(1, self.big):
                    to = (lax.rem(self.z + k, self.big) * 2 + self.y, self.d)
                    self.go(part, self.send_b.at[t, k], self.have.at[t, 2 + self.z], to)
            part = self.buf.at[e, self.rows_pair(self.y)]
            self.pass_on(part, t, self.y)
            if self.r2:
                self.pass_on(self.buf.at[e, self.rows_many(self.z)], t, 2 + self.z)

    def pass_on(self, part, t, c):
        self.go(part, self.send_c.at[t, c], self.partner_have.at[t, c], (self.s, self.partner))

    def collect(self):
        for t in self.mirrors:
            e = self.source(t)
            c = 1 - self.y
            part = self.buf.at[e, self.rows_pair(c)]
            self.take(part, self.have.at[t, c])
            self.pass_on(part, t, c)
            if self.r2:
                for k in range(1, self.big):
                    c = lax.rem(self.z + k, self.big)
                    part = self.buf.at[e, self.rows_many(c)]
                    self.take(part, self.have.at[t, 2 + c])
                    self.pass_on(part, t, 2 + c)

    def finish(self, t):
        e = self.source(t)
        other = e + 1 - 2 * lax.rem(e, 2)
        for c in range(2):
            self.take(self.buf.at[other, self.rows_pair(c)], self.partner_have.at[t, c])
        if self.r2:
            for c in range(self.big):
                self.take(self.buf.at[other, self.rows_many(c)], self.partner_have.at[t, 2 + c])
        return other

    def drain(self):
        for copy in self.started:
            copy.wait_send()


def split_rows(rows, n):
    big = n // 2
    many = rows * 5 // 8 // big // 16 * 16
    return (rows - many * big) // 2, many


def gather_sems(n, m):
    dma = pltpu.SemaphoreType.DMA
    t, c = max(m // 2, 2), 2 + n // 2
    return [dma((t, c)), dma((t, c)), dma, dma((t, 2)), dma((t, max(2, n // 2))), dma((t, c)), dma]


def layer_kernel(n, m, sequences, heads, pairs, hidden, gates, wq, wk, wv, wo, out,
                 qkv, outw, summed, send, got, gate_got, gate_row, gate_column, keys, values, att, ret, lhs, *sems):
    s, d = lax.axis_index("sp"), lax.axis_index("dp")
    first, second = sems[:7], sems[7:14]
    local, gate_send, gate_recv, q_send, q_recv, r_send, r_recv = sems[14:]
    positions = hidden.shape[0] // sequences
    length = positions * n
    mesh_id = pl.DeviceIdType.MESH
    one = Gather(qkv, n, m, (s, d), first)
    two = Gather(outw, n, m, (s, d), second)
    width_q, width_k = wq.shape[1], wk.shape[1]

    inward = [
        pltpu.make_async_copy(wq, qkv.at[d, :, pl.ds(0, width_q)], local.at[0]),
        pltpu.make_async_copy(wk, qkv.at[d, :, pl.ds(width_q, width_k)], local.at[1]),
        pltpu.make_async_copy(wv, qkv.at[d, :, pl.ds(width_q + width_k, width_k)], local.at[2]),
        pltpu.make_async_copy(wo, outw.at[d], local.at[3]),
        pltpu.make_async_copy(gates.at[s], gate_got.at[s], local.at[4]),
    ]
    for copy in inward:
        copy.start()
    barrier = pltpu.get_barrier_semaphore()
    for k in range(1, n):
        pl.semaphore_signal(barrier, inc=1, device_id=(lax.rem(s + k, n), d), device_id_type=mesh_id)
    for k in range(1, m):
        pl.semaphore_signal(barrier, inc=1, device_id=(s, lax.rem(d + k, m)), device_id_type=mesh_id)
    pl.semaphore_wait(barrier, n - 1 + m - 1)

    def exchange(source, target, send_sem, recv_sem):
        copies = []
        for k in range(1, n):
            to = lax.rem(s + k, n)
            copy = pltpu.make_async_remote_copy(
                src_ref=source(to), dst_ref=target(s), send_sem=send_sem(k), recv_sem=recv_sem(n - k),
                device_id=(to, d), device_id_type=mesh_id,
            )
            copy.start()
            copies.append(copy)
        return copies

    def arrive(target, send_sem, recv_sem):
        for k in range(1, n):
            block = target(lax.rem(s + k, n))
            pltpu.make_async_remote_copy(
                src_ref=block, dst_ref=block, send_sem=send_sem(k), recv_sem=recv_sem(k),
                device_id=(lax.rem(s + k, n), d), device_id_type=mesh_id,
            ).wait_recv()

    for copy in inward[:3]:
        copy.wait()
    one.cross()
    one.to_partner()
    gate_args = lambda j: gates.at[j], lambda j: gate_got.at[j], lambda k: gate_send.at[k], lambda k: gate_recv.at[k]
    gate_copies = exchange(*gate_args)

    depth = qkv.shape[1]
    tile = math.gcd(qkv.shape[2], 512)

    def project(e, begin):
        columns = hidden[:, pl.ds(pl.multiple_of(e * depth, 128), depth)]

        def step(c, nothing):
            at = pl.ds(pl.multiple_of(c * tile, tile), tile)
            product = jnp.dot(columns, qkv[e, :, at], preferred_element_type=jnp.float32)
            summed[:, at] = product if begin else summed[:, at] + product
            return nothing

        lax.fori_loop(0, qkv.shape[2] // tile, step, 0)

    project(d, True)
    one.take_partner()
    project(one.partner, False)
    one.share()
    for copy in inward[3:]:
        copy.wait()
    two.cross()
    two.to_partner()
    one.collect()
    for t in one.mirrors:
        project(one.source(t), False)
        project(one.finish(t), False)

    width = heads * HEAD
    across = n * pairs * HEAD // width_k
    for j in range(n):
        send[j, :, :width] = summed[:, j * width : (j + 1) * width].astype(jnp.bfloat16)
        at = width_q + (j // across) * pairs * HEAD
        send[j, :, width : width + pairs * HEAD] = summed[:, at : at + pairs * HEAD].astype(jnp.bfloat16)
        at = at + width_k
        send[j, :, width + pairs * HEAD :] = summed[:, at : at + pairs * HEAD].astype(jnp.bfloat16)
    own = pltpu.make_async_copy(send.at[s], got.at[s], local.at[5])
    own.start()
    q_args = lambda j: send.at[j], lambda j: got.at[j], lambda k: q_send.at[k], lambda k: q_recv.at[k]
    q_copies = exchange(*q_args)
    two.share()
    arrive(*gate_args[1:])
    for j in range(n):
        gate_row[:, j * positions : (j + 1) * positions] = gate_got[j]
    gate_column[...] = jnp.transpose(gate_row[...])
    own.wait()
    arrive(*q_args[1:])

    rows = math.gcd(length, 256)
    own_copies, r_copies = [], []
    for q in range(sequences):
        top = q * positions
        for j in range(n):
            part = got[j, top : top + positions, width : width + pairs * HEAD]
            keys[j * positions : (j + 1) * positions, :] = part
            values[j * positions : (j + 1) * positions, :] = got[j, top : top + positions, width + pairs * HEAD :]
        blocks = rows // positions
        for head in range(heads):
            lanes = slice(head * HEAD, (head + 1) * HEAD)
            pair = head * pairs // heads
            kv = slice(pair * HEAD, (pair + 1) * HEAD)
            gate = q * heads + head

            def q_of(start, count):
                return got[pl.ds(start // positions, count // positions), top : top + positions, lanes].reshape(
                    count, HEAD
                )

            def store(block, value):
                att[q, pl.ds(block * blocks, blocks), :, lanes] = value.reshape(blocks, positions, HEAD)

            if length <= 1024:
                for block in range(length // rows):
                    start = block * rows
                    store(block, attend_rows(
                        q_of(start, rows),
                        lambda lo, hi: keys[lo:hi, kv],
                        lambda lo, hi: values[lo:hi, kv],
                        gate_column[start : start + rows, gate : gate + 1],
                        lambda lo, hi: gate_row[gate : gate + 1, lo:hi],
                        start,
                        rows,
                    ))
            else:
                attend_long(
                    q_of,
                    lambda lo, count: keys[pl.ds(lo, count), kv],
                    lambda lo, count: values[pl.ds(lo, count), kv],
                    lambda lo, count: gate_column[pl.ds(lo, count), gate : gate + 1],
                    lambda lo, count: gate_row[gate : gate + 1, pl.ds(lo, count)],
                    store,
                    length,
                    rows,
                )
        copy = pltpu.make_async_copy(att.at[q, s], ret.at[q, s], local.at[6 + q])
        copy.start()
        own_copies.append(copy)
        r_copies += exchange(
            lambda j: att.at[q, j], lambda j: ret.at[q, j], lambda k: r_send.at[q, k], lambda k: r_recv.at[q, k]
        )
        if q == 0:
            two.take_partner()
            two.collect()
    for t in two.mirrors:
        two.finish(t)
    for q in range(sequences):
        own_copies[q].wait()
        arrive(lambda j: ret.at[q, j], lambda k: r_send.at[q, k], lambda k: r_recv.at[q, k])
        for j in range(n):
            lhs[q * positions : (q + 1) * positions, j * width : (j + 1) * width] = ret[q, j]

    depth_out = outw.shape[1]
    tile_out = math.gcd(outw.shape[2], 256)

    def produce(c, nothing):
        at = pl.ds(pl.multiple_of(c * tile_out, tile_out), tile_out)
        total = jnp.dot(lhs[:, :depth_out], outw[0, :, at], preferred_element_type=jnp.float32)
        for e in range(1, m):
            block = lhs[:, e * depth_out : (e + 1) * depth_out]
            total = total + jnp.dot(block, outw[e, :, at], preferred_element_type=jnp.float32)
        out[:, at] = total.astype(jnp.bfloat16)
        return nothing

    lax.fori_loop(0, outw.shape[2] // tile_out, produce, 0)
    one.drain()
    two.drain()
    for copy in gate_copies + q_copies + r_copies:
        copy.wait_send()


def on_device(n, m, hidden_states, cumulative_gate, query_weight, key_weight, value_weight, out_weight):
    sequences, positions, model_width = hidden_states.shape
    count = sequences * positions
    all_heads = cumulative_gate.shape[2]
    heads = all_heads // n
    copies = max(1, n // KV_HEADS)
    pairs = KV_HEADS * copies // n
    length = positions * n
    gates = jnp.transpose(cumulative_gate.reshape(sequences, positions, n, heads), (2, 0, 3, 1))
    gates = gates.reshape(n, sequences * heads, positions)
    lines = -(-sequences * heads // 8) * 8
    gates = jnp.pad(gates, ((0, 0), (0, lines - sequences * heads), (0, 0)))
    width = heads * HEAD
    wide = query_weight.shape[1] + 2 * key_weight.shape[1]
    shard = query_weight.shape[0]
    dma, bf, f32 = pltpu.SemaphoreType.DMA, jnp.bfloat16, jnp.float32
    vmem, anywhere = pl.BlockSpec(memory_space=pltpu.VMEM), pl.BlockSpec(memory_space=pl.ANY)
    mixed = pl.pallas_call(
        functools.partial(layer_kernel, n, m, sequences, heads, pairs),
        out_shape=jax.ShapeDtypeStruct((count, model_width), bf),
        in_specs=[vmem, vmem] + [anywhere] * 4,
        out_specs=vmem,
        scratch_shapes=[
            pltpu.VMEM((m, shard, wide), bf),
            pltpu.VMEM((m, out_weight.shape[0], model_width), bf),
            pltpu.VMEM((count, wide), f32),
            pltpu.VMEM((n, count, width + 2 * pairs * HEAD), bf),
            pltpu.VMEM((n, count, width + 2 * pairs * HEAD), bf),
            pltpu.VMEM((n, lines, positions), f32),
            pltpu.VMEM((lines, length), f32),
            pltpu.VMEM((length, lines), f32),
            pltpu.VMEM((length, pairs * HEAD), bf),
            pltpu.VMEM((length, pairs * HEAD), bf),
            pltpu.VMEM((sequences, n, positions, width), bf),
            pltpu.VMEM((sequences, n, positions, width), bf),
            pltpu.VMEM((count, out_weight.shape[0] * m), bf),
            *gather_sems(n, m),
            *gather_sems(n, m),
            dma((6 + sequences,)),
            dma((n,)),
            dma((n,)),
            dma((n,)),
            dma((n,)),
            dma((sequences, n)),
            dma((sequences, n)),
        ],
        compiler_params=pltpu.CompilerParams(
            collective_id=0, has_side_effects=True, vmem_limit_bytes=60 * 1024 * 1024
        ),
    )(
        hidden_states.reshape(count, model_width), gates, query_weight, key_weight, value_weight, out_weight
    )
    return mixed.reshape(sequences, positions, model_width)


def solution(mesh):
    placed = (
        P("dp", "sp", None),
        P("dp", "sp", None),
        P("dp", None),
        P("dp", None),
        P("dp", None),
        P("dp", None),
    )
    return jax.shard_map(
        functools.partial(on_device, mesh.shape["sp"], mesh.shape["dp"]),
        mesh=mesh, in_specs=placed, out_specs=P("dp", "sp", None), check_vma=False,
    )
```

```python
import functools
import math

import jax
import jax.numpy as jnp
from jax import lax
from jax.experimental import pallas as pl
from jax.experimental.pallas import tpu as pltpu
from jax.sharding import PartitionSpec as P

KV_HEADS = 8
HEAD = 64
SHARE_KV, SHARE_Q, SHARE_OUT = 3, 2, 0


def attend_rows(q, k_of, v_of, gate_column, gate_row_of, start, rows):
    scaled = q * jnp.asarray(HEAD**-0.5, q.dtype)
    contract = (((1,), (1,)), ((), ()))

    def scores(lo, hi):
        product = lax.dot_general(scaled, k_of(lo, hi), contract, preferred_element_type=jnp.float32)
        return product + (gate_column - gate_row_of(lo, hi))

    diagonal = scores(start, start + rows)
    row = lax.broadcasted_iota(jnp.int32, diagonal.shape, 0)
    column = lax.broadcasted_iota(jnp.int32, diagonal.shape, 1)
    diagonal = jnp.where(column <= row, diagonal, -jnp.inf)
    top = jnp.max(diagonal, axis=1, keepdims=True)
    if start:
        before = scores(0, start)
        top = jnp.maximum(top, jnp.max(before, axis=1, keepdims=True))
    raised = jnp.exp(diagonal - top)
    total = jnp.sum(raised, axis=1, keepdims=True)
    mixed = jnp.dot(raised.astype(jnp.bfloat16), v_of(start, start + rows), preferred_element_type=jnp.float32)
    if start:
        raised = jnp.exp(before - top)
        total = total + jnp.sum(raised, axis=1, keepdims=True)
        mixed = mixed + jnp.dot(raised.astype(jnp.bfloat16), v_of(0, start), preferred_element_type=jnp.float32)
    return (mixed / total).astype(jnp.bfloat16)


def attend_long(q_of, k_of, v_of, gate_column_of, gate_row_of, store, length, rows):
    contract = (((1,), (1,)), ((), ()))

    def one_block(block, nothing):
        start = pl.multiple_of(block * rows, rows)
        q = q_of(start, rows)
        scaled = q * jnp.asarray(HEAD**-0.5, q.dtype)
        column = gate_column_of(start, rows)

        def step(other, carry):
            top, total, mixed = carry
            lo = pl.multiple_of(other * rows, rows)
            s = lax.dot_general(scaled, k_of(lo, rows), contract, preferred_element_type=jnp.float32)
            s = s + (column - gate_row_of(lo, rows))
            at = lax.broadcasted_iota(jnp.int32, s.shape, 0) + start
            to = lax.broadcasted_iota(jnp.int32, s.shape, 1) + lo
            s = jnp.where(to <= at, s, -jnp.inf)
            new = jnp.maximum(top, jnp.max(s, axis=1, keepdims=True))
            raised = jnp.exp(s - new)
            keep = jnp.exp(top - new)
            total = total * keep + jnp.sum(raised, axis=1, keepdims=True)
            part = jnp.dot(raised.astype(jnp.bfloat16), v_of(lo, rows), preferred_element_type=jnp.float32)
            return new, total, mixed * keep + part

        first = (
            jnp.full((rows, 1), -jnp.inf, jnp.float32),
            jnp.zeros((rows, 1), jnp.float32),
            jnp.zeros((rows, HEAD), jnp.float32),
        )
        _, total, mixed = lax.fori_loop(0, block + 1, step, first)
        store(block, (mixed / total).astype(jnp.bfloat16))
        return nothing

    lax.fori_loop(0, length // rows, one_block, 0)


class Gather:
    def __init__(self, buf, n, m, me, sems, eighths):
        self.buf, self.n, self.m = buf, n, m
        self.s, self.d = me
        self.have, self.partner_have, self.own_recv, self.send_a, self.send_b, self.send_c, self.own_send = sems
        self.partner = self.d + 1 - 2 * lax.rem(self.d, 2)
        self.y, self.z = lax.rem(self.s, 2), self.s // 2
        self.big = n // 2
        self.r1, self.r2 = split_rows(buf.shape[1], n, eighths)
        self.started = []
        self.mirrors = range(1, m // 2)

    def rows_pair(self, y):
        return pl.ds(pl.multiple_of(y * self.r1, 16), self.r1)

    def rows_many(self, z):
        return pl.ds(pl.multiple_of(2 * self.r1 + z * self.r2, 16), self.r2)

    def go(self, part, send, recv, device):
        copy = pltpu.make_async_remote_copy(
            src_ref=part, dst_ref=part, send_sem=send, recv_sem=recv, device_id=device,
            device_id_type=pl.DeviceIdType.MESH,
        )
        copy.start()
        self.started.append(copy)

    def take(self, part, recv):
        pltpu.make_async_remote_copy(
            src_ref=part, dst_ref=part, send_sem=self.own_send, recv_sem=recv, device_id=(self.s, self.partner),
            device_id_type=pl.DeviceIdType.MESH,
        ).wait_recv()

    def cross(self):
        for t in self.mirrors:
            to = (self.s, lax.rem(self.d + 2 * t, self.m))
            self.go(self.buf.at[self.d, self.rows_pair(self.y)], self.send_a.at[t, 0], self.have.at[t, self.y], to)
            if self.r2:
                self.go(
                    self.buf.at[self.d, self.rows_many(self.z)], self.send_a.at[t, 1], self.have.at[t, 2 + self.z], to
                )

    def to_partner(self):
        self.go(self.buf.at[self.d], self.own_send, self.own_recv, (self.s, self.partner))

    def take_partner(self):
        self.take(self.buf.at[self.partner], self.own_recv)

    def source(self, t):
        return lax.rem(self.d - 2 * t + self.m, self.m)

    def share(self):
        for t in self.mirrors:
            e = self.source(t)
            part = self.buf.at[e, self.rows_pair(self.y)]
            self.take(part, self.have.at[t, self.y])
            self.go(part, self.send_b.at[t, 0], self.have.at[t, self.y], (self.s + 1 - 2 * self.y, self.d))
            if self.r2:
                part = self.buf.at[e, self.rows_many(self.z)]
                self.take(part, self.have.at[t, 2 + self.z])
                for k in range(1, self.big):
                    to = (lax.rem(self.z + k, self.big) * 2 + self.y, self.d)
                    self.go(part, self.send_b.at[t, k], self.have.at[t, 2 + self.z], to)
            part = self.buf.at[e, self.rows_pair(self.y)]
            self.pass_on(part, t, self.y)
            if self.r2:
                self.pass_on(self.buf.at[e, self.rows_many(self.z)], t, 2 + self.z)

    def pass_on(self, part, t, c):
        self.go(part, self.send_c.at[t, c], self.partner_have.at[t, c], (self.s, self.partner))

    def collect(self):
        for t in self.mirrors:
            e = self.source(t)
            c = 1 - self.y
            part = self.buf.at[e, self.rows_pair(c)]
            self.take(part, self.have.at[t, c])
            self.pass_on(part, t, c)
            if self.r2:
                for k in range(1, self.big):
                    c = lax.rem(self.z + k, self.big)
                    part = self.buf.at[e, self.rows_many(c)]
                    self.take(part, self.have.at[t, 2 + c])
                    self.pass_on(part, t, 2 + c)

    def finish(self, t):
        e = self.source(t)
        other = e + 1 - 2 * lax.rem(e, 2)
        for c in range(2):
            self.take(self.buf.at[other, self.rows_pair(c)], self.partner_have.at[t, c])
        if self.r2:
            for c in range(self.big):
                self.take(self.buf.at[other, self.rows_many(c)], self.partner_have.at[t, 2 + c])
        return other

    def drain(self):
        for copy in self.started:
            copy.wait_send()


def split_rows(rows, n, eighths):
    big = n // 2
    many = rows * eighths // 8 // big // 16 * 16
    return (rows - many * big) // 2, many


def gather_sems(n, m):
    dma = pltpu.SemaphoreType.DMA
    t, c = max(m // 2, 2), 2 + n // 2
    return [dma((t, c)), dma((t, c)), dma, dma((t, 2)), dma((t, max(2, n // 2))), dma((t, c)), dma]


def layer_kernel(n, m, sequences, heads, pairs, hidden, gates, wq, wk, wv, wo, out,
                 kvw, qw, outw, summed_kv, summed_q, send_kv, got_kv, send, got, gate_got, gate_row, gate_column, keys, values, att, ret, lhs, *sems):
    s, d = lax.axis_index("sp"), lax.axis_index("dp")
    local, gate_send, gate_recv, kv_send, kv_recv, q_send, q_recv, r_send, r_recv = sems[21:]
    positions = hidden.shape[0] // sequences
    length = positions * n
    mesh_id = pl.DeviceIdType.MESH
    zero = Gather(kvw, n, m, (s, d), sems[:7], SHARE_KV)
    one = Gather(qw, n, m, (s, d), sems[7:14], SHARE_Q)
    two = Gather(outw, n, m, (s, d), sems[14:21], SHARE_OUT)
    width_k = wk.shape[1]

    inward = [
        pltpu.make_async_copy(wk, kvw.at[d, :, pl.ds(0, width_k)], local.at[0]),
        pltpu.make_async_copy(wv, kvw.at[d, :, pl.ds(width_k, width_k)], local.at[1]),
        pltpu.make_async_copy(wq, qw.at[d], local.at[2]),
        pltpu.make_async_copy(wo, outw.at[d], local.at[3]),
        pltpu.make_async_copy(gates.at[s], gate_got.at[s], local.at[4]),
    ]
    for copy in inward:
        copy.start()
    barrier = pltpu.get_barrier_semaphore()
    for k in range(1, n):
        pl.semaphore_signal(barrier, inc=1, device_id=(lax.rem(s + k, n), d), device_id_type=mesh_id)
    for k in range(1, m):
        pl.semaphore_signal(barrier, inc=1, device_id=(s, lax.rem(d + k, m)), device_id_type=mesh_id)
    pl.semaphore_wait(barrier, n - 1 + m - 1)

    def exchange(source, target, send_sem, recv_sem):
        copies = []
        for k in range(1, n):
            to = lax.rem(s + k, n)
            copy = pltpu.make_async_remote_copy(
                src_ref=source(to), dst_ref=target(s), send_sem=send_sem(k), recv_sem=recv_sem(n - k),
                device_id=(to, d), device_id_type=mesh_id,
            )
            copy.start()
            copies.append(copy)
        return copies

    def arrive(target, send_sem, recv_sem):
        for k in range(1, n):
            block = target(lax.rem(s + k, n))
            pltpu.make_async_remote_copy(
                src_ref=block, dst_ref=block, send_sem=send_sem(k), recv_sem=recv_sem(k),
                device_id=(lax.rem(s + k, n), d), device_id_type=mesh_id,
            ).wait_recv()

    inward[0].wait()
    inward[1].wait()
    zero.cross()
    zero.to_partner()
    inward[2].wait()
    one.cross()
    one.to_partner()
    inward[4].wait()
    gate_args = lambda j: gates.at[j], lambda j: gate_got.at[j], lambda k: gate_send.at[k], lambda k: gate_recv.at[k]
    gate_copies = exchange(*gate_args)
    inward[3].wait()
    two.cross()

    depth = qw.shape[1]

    def project(weight, summed, e, begin):
        tile = math.gcd(weight.shape[2], 512)
        columns = hidden[:, pl.ds(pl.multiple_of(e * depth, 128), depth)]

        def step(c, nothing):
            at = pl.ds(pl.multiple_of(c * tile, tile), tile)
            product = jnp.dot(columns, weight[e, :, at], preferred_element_type=jnp.float32)
            summed[:, at] = product if begin else summed[:, at] + product
            return nothing

        lax.fori_loop(0, weight.shape[2] // tile, step, 0)

    project(kvw, summed_kv, d, True)
    zero.take_partner()
    project(kvw, summed_kv, zero.partner, False)
    project(qw, summed_q, d, True)
    zero.share()
    zero.collect()
    for t in zero.mirrors:
        project(kvw, summed_kv, zero.source(t), False)
        project(kvw, summed_kv, zero.finish(t), False)

    width, thin = heads * HEAD, pairs * HEAD
    across = n * thin // width_k
    for j in range(n):
        at = (j // across) * thin
        send_kv[j, :, :thin] = summed_kv[:, at : at + thin].astype(jnp.bfloat16)
        send_kv[j, :, thin:] = summed_kv[:, width_k + at : width_k + at + thin].astype(jnp.bfloat16)
    own_kv = pltpu.make_async_copy(send_kv.at[s], got_kv.at[s], local.at[5])
    own_kv.start()
    kv_args = lambda j: send_kv.at[j], lambda j: got_kv.at[j], lambda k: kv_send.at[k], lambda k: kv_recv.at[k]
    kv_copies = exchange(*kv_args)

    one.take_partner()
    project(qw, summed_q, one.partner, False)
    one.share()
    two.to_partner()
    one.collect()
    for t in one.mirrors:
        project(qw, summed_q, one.source(t), False)
        project(qw, summed_q, one.finish(t), False)
    q_copies, own_q = [], []

    def q_args(q):
        part = pl.ds(q * positions, positions)
        return (
            lambda j: send.at[j, part],
            lambda j: got.at[j, part],
            lambda k: q_send.at[q, k],
            lambda k: q_recv.at[q, k],
        )

    for q in range(sequences):
        lines = slice(q * positions, (q + 1) * positions)
        for j in range(n):
            send[j, lines, :] = summed_q[lines, j * width : (j + 1) * width].astype(jnp.bfloat16)
        copy = pltpu.make_async_copy(q_args(q)[0](s), q_args(q)[1](s), local.at[6 + q])
        copy.start()
        own_q.append(copy)
        q_copies += exchange(*q_args(q))
    arrive(*gate_args[1:])
    for j in range(n):
        gate_row[:, j * positions : (j + 1) * positions] = gate_got[j]
    gate_column[...] = jnp.transpose(gate_row[...])
    own_kv.wait()
    arrive(*kv_args[1:])

    rows = math.gcd(length, 256)
    own_copies, r_copies = [], []
    for q in range(sequences):
        top = q * positions
        for j in range(n):
            keys[j * positions : (j + 1) * positions, :] = got_kv[j, top : top + positions, :thin]
            values[j * positions : (j + 1) * positions, :] = got_kv[j, top : top + positions, thin:]
        own_q[q].wait()
        arrive(*q_args(q)[1:])
        if q == 0:
            two.share()
        blocks = rows // positions
        for head in range(heads):
            lanes = slice(head * HEAD, (head + 1) * HEAD)
            pair = head * pairs // heads
            kv = slice(pair * HEAD, (pair + 1) * HEAD)
            gate = q * heads + head

            def q_of(start, count):
                return got[pl.ds(start // positions, count // positions), top : top + positions, lanes].reshape(
                    count, HEAD
                )

            def store(block, value):
                att[q, pl.ds(block * blocks, blocks), :, lanes] = value.reshape(blocks, positions, HEAD)

            if length <= 1024:
                for block in range(length // rows):
                    start = block * rows
                    store(block, attend_rows(
                        q_of(start, rows),
                        lambda lo, hi: keys[lo:hi, kv],
                        lambda lo, hi: values[lo:hi, kv],
                        gate_column[start : start + rows, gate : gate + 1],
                        lambda lo, hi: gate_row[gate : gate + 1, lo:hi],
                        start,
                        rows,
                    ))
            else:
                attend_long(
                    q_of,
                    lambda lo, count: keys[pl.ds(lo, count), kv],
                    lambda lo, count: values[pl.ds(lo, count), kv],
                    lambda lo, count: gate_column[pl.ds(lo, count), gate : gate + 1],
                    lambda lo, count: gate_row[gate : gate + 1, pl.ds(lo, count)],
                    store,
                    length,
                    rows,
                )
        copy = pltpu.make_async_copy(att.at[q, s], ret.at[q, s], local.at[6 + sequences + q])
        copy.start()
        own_copies.append(copy)
        r_copies += exchange(
            lambda j: att.at[q, j], lambda j: ret.at[q, j], lambda k: r_send.at[q, k], lambda k: r_recv.at[q, k]
        )
    two.take_partner()
    two.collect()
    for t in two.mirrors:
        two.finish(t)
    for q in range(sequences):
        own_copies[q].wait()
        arrive(lambda j: ret.at[q, j], lambda k: r_send.at[q, k], lambda k: r_recv.at[q, k])
        for j in range(n):
            lhs[q * positions : (q + 1) * positions, j * width : (j + 1) * width] = ret[q, j]

    depth_out = outw.shape[1]
    tile_out = math.gcd(outw.shape[2], 256)

    def produce(c, nothing):
        at = pl.ds(pl.multiple_of(c * tile_out, tile_out), tile_out)
        total = jnp.dot(lhs[:, :depth_out], outw[0, :, at], preferred_element_type=jnp.float32)
        for e in range(1, m):
            block = lhs[:, e * depth_out : (e + 1) * depth_out]
            total = total + jnp.dot(block, outw[e, :, at], preferred_element_type=jnp.float32)
        out[:, at] = total.astype(jnp.bfloat16)
        return nothing

    lax.fori_loop(0, outw.shape[2] // tile_out, produce, 0)
    zero.drain()
    one.drain()
    two.drain()
    for copy in gate_copies + kv_copies + q_copies + r_copies:
        copy.wait_send()


def on_device(n, m, hidden_states, cumulative_gate, query_weight, key_weight, value_weight, out_weight):
    sequences, positions, model_width = hidden_states.shape
    count = sequences * positions
    all_heads = cumulative_gate.shape[2]
    heads = all_heads // n
    copies = max(1, n // KV_HEADS)
    pairs = KV_HEADS * copies // n
    length = positions * n
    gates = jnp.transpose(cumulative_gate.reshape(sequences, positions, n, heads), (2, 0, 3, 1))
    gates = gates.reshape(n, sequences * heads, positions)
    lines = -(-sequences * heads // 8) * 8
    gates = jnp.pad(gates, ((0, 0), (0, lines - sequences * heads), (0, 0)))
    width = heads * HEAD
    wide, narrow = query_weight.shape[1], 2 * key_weight.shape[1]
    shard = query_weight.shape[0]
    dma, bf, f32 = pltpu.SemaphoreType.DMA, jnp.bfloat16, jnp.float32
    vmem, anywhere = pl.BlockSpec(memory_space=pltpu.VMEM), pl.BlockSpec(memory_space=pl.ANY)
    mixed = pl.pallas_call(
        functools.partial(layer_kernel, n, m, sequences, heads, pairs),
        out_shape=jax.ShapeDtypeStruct((count, model_width), bf),
        in_specs=[vmem, vmem] + [anywhere] * 4,
        out_specs=vmem,
        scratch_shapes=[
            pltpu.VMEM((m, shard, narrow), bf),
            pltpu.VMEM((m, shard, wide), bf),
            pltpu.VMEM((m, out_weight.shape[0], model_width), bf),
            pltpu.VMEM((count, narrow), f32),
            pltpu.VMEM((count, wide), f32),
            pltpu.VMEM((n, count, 2 * pairs * HEAD), bf),
            pltpu.VMEM((n, count, 2 * pairs * HEAD), bf),
            pltpu.VMEM((n, count, width), bf),
            pltpu.VMEM((n, count, width), bf),
            pltpu.VMEM((n, lines, positions), f32),
            pltpu.VMEM((lines, length), f32),
            pltpu.VMEM((length, lines), f32),
            pltpu.VMEM((length, pairs * HEAD), bf),
            pltpu.VMEM((length, pairs * HEAD), bf),
            pltpu.VMEM((sequences, n, positions, width), bf),
            pltpu.VMEM((sequences, n, positions, width), bf),
            pltpu.VMEM((count, out_weight.shape[0] * m), bf),
            *gather_sems(n, m),
            *gather_sems(n, m),
            *gather_sems(n, m),
            dma((6 + 2 * sequences,)),
            dma((n,)),
            dma((n,)),
            dma((n,)),
            dma((n,)),
            dma((sequences, n)),
            dma((sequences, n)),
            dma((sequences, n)),
            dma((sequences, n)),
        ],
        compiler_params=pltpu.CompilerParams(
            collective_id=0, has_side_effects=True, vmem_limit_bytes=60 * 1024 * 1024
        ),
    )(
        hidden_states.reshape(count, model_width), gates, query_weight, key_weight, value_weight, out_weight
    )
    return mixed.reshape(sequences, positions, model_width)


def solution(mesh):
    placed = (
        P("dp", "sp", None),
        P("dp", "sp", None),
        P("dp", None),
        P("dp", None),
        P("dp", None),
        P("dp", None),
    )
    return jax.shard_map(
        functools.partial(on_device, mesh.shape["sp"], mesh.shape["dp"]),
        mesh=mesh, in_specs=placed, out_specs=P("dp", "sp", None), check_vma=False,
    )
```
